32 devices in a mesh: kv: 8 (over z, x), tp: 4 (over y, core).
Axes of the slice: x: 2, y: 2, z: 4, core: 2. Of those that a mesh axis runs over, the one named last changes fastest.
Arguments:
- hidden_rows: bfloat16 [28, 4096], P(None, ('kv', 'tp')), may hold values from -6 to 6
- first_gain: float32 [4096], P('kv'), may hold values from 0.1 to 1.9
- first_gate: bfloat16 [4096, 11264], P('kv', 'tp'), may hold values from -0.125 to 0.125
- first_up: bfloat16 [4096, 11264], P('kv', 'tp'), may hold values from -0.125 to 0.125
- first_down: bfloat16 [11264, 4096], P('tp', 'kv'), may hold values from -0.078125 to 0.078125
- mix_gain: float32 [4096], P('kv'), may hold values from 0.1 to 1.9
- query_weight: bfloat16 [4096, 2048], P('kv', 'tp'), may hold values from -0.09375 to 0.09375
- key_weight: bfloat16 [4096, 2048], P('kv', 'tp'), may hold values from -0.09375 to 0.09375
- value_weight: bfloat16 [4096, 2048], P('kv', 'tp'), may hold values from -0.09375 to 0.09375
- forget_weight: bfloat16 [4096, 16], P('kv'), may hold values from -0.09375 to 0.09375
- forget_bias: float32 [16], replicated, may hold values from -8 to 2
- out_weight: bfloat16 [2048, 4096], P('tp', 'kv'), may hold values from -0.5 to 0.5
- second_gain: float32 [4096], P('kv'), may hold values from 0.1 to 1.9
- second_gate: bfloat16 [4096, 11264], P('kv', 'tp'), may hold values from -0.125 to 0.125
- second_up: bfloat16 [4096, 11264], P('kv', 'tp'), may hold values from -0.125 to 0.125
- second_down: bfloat16 [11264, 4096], P('tp', 'kv'), may hold values from -0.078125 to 0.078125
- cache_keys: bfloat16 [28, 2048, 2048], P(None, 'kv', 'tp'), may hold values from -48 to 48
- cache_values: bfloat16 [28, 2048, 2048], P(None, 'kv', 'tp'), may hold values from -6 to 6
- cache_gates: float32 [28, 16, 2048], P(None, 'tp', 'kv'), may hold values from -1 to 0
- lengths: int32 [28], replicated, may hold values from 1 to 2048, 16384 in all
Outputs:
- out_rows: bfloat16 [28, 4096], P(None, ('kv', 'tp'))
The draws below stay inside these ranges and needn't reach their ends.
Inputs may be any that keep to these rules, and one draw needn't show every extreme that they name: Sequence b uses cache positions 0 to lengths[b] - 1; some sequence uses all 2048.
All inputs are finite; a program needn't handle non-finite values.
Results may differ from the reference program's by a relative error of at most 0.014.
Values may be sent and summed in bfloat16 or wider, within the bound.
A program may use at most 128 MiB of HBM per device.

```python
import math
import jax
import jax.numpy as jnp
import numpy as np
from jax import lax

D = 4096
FF = 11264
HEADS = 16
HEAD_DIM = 128
SEQS = 28
POS_DEV = 256
LENGTH = 2048


def draw_cache_keys(key, part):
    base = jax.random.normal(jax.random.fold_in(key, 11), (SEQS, LENGTH, HEADS, HEAD_DIM), jnp.float32)
    base = jnp.clip(base, -48.0, 48.0)
    return base.reshape(SEQS, LENGTH, HEADS * HEAD_DIM).astype(jnp.bfloat16)


def draw_cache_gates(key, part):
    fast_share = 0.5
    fast = jax.random.uniform(jax.random.fold_in(key, 21), (HEADS,)) < fast_share
    fast_rate = jnp.exp(jax.random.uniform(jax.random.fold_in(key, 22), (HEADS,), jnp.float32, math.log(1.0 / 100.0), math.log(1.0 / 30.0)))
    slow_rate = jnp.exp(jax.random.uniform(jax.random.fold_in(key, 23), (HEADS,), jnp.float32, math.log(0.5), math.log(1.0))) / LENGTH
    rate = jnp.where(fast, fast_rate, slow_rate)
    spread = jnp.where(fast, math.log(4.0), math.log(10.0))
    coords = jax.random.uniform(jax.random.fold_in(key, 24), (SEQS, HEADS, LENGTH // POS_DEV), jnp.float32, -1.0, 1.0)
    block_factor = jnp.exp(coords * spread[None, :, None])
    block_factor = jnp.repeat(block_factor, POS_DEV, axis=2)
    noise = jax.random.uniform(jax.random.fold_in(key, 25), (SEQS, HEADS, LENGTH), jnp.float32, 0.5, 1.5)
    values = -(rate[None, :, None] * block_factor * noise)
    return jnp.clip(values, -1.0, 0.0)


def strengthened(drawn, own_key, source, target, shards_of, factor):
    owner, partner = [(jnp.arange(drawn.shape[dim]) // (drawn.shape[dim] // shards_of)).reshape([-1 if axis == dim else 1 for axis in range(drawn.ndim)]) for dim in (source, target)]
    chosen = jax.random.permutation(own_key, shards_of)[partner]
    strong = (owner == chosen) | (owner == (partner + shards_of // 2) % shards_of)
    return jnp.where(strong, factor * drawn, drawn)


def level_of(rng, extent, pieces, smallest, top_value):
    level, own = 1.0, jax.random.fold_in(rng, 6)
    for axis_at, shards_of in pieces:
        heights = jnp.exp(jax.random.uniform(jax.random.fold_in(own, axis_at), (shards_of,), jnp.float32, smallest / len(pieces), top_value / len(pieces)))
        level = level * jnp.repeat(heights, extent[axis_at] // shards_of).reshape([-1 if axis == axis_at else 1 for axis in range(len(extent))])
    return level


def split_up(number_of, total, most, lean):
    loads = [(1 << 20) // math.isqrt(standing ** lean) + 1 for standing in range(2, number_of + 1)]
    rest, counts = total - most - (number_of - 1), [1] * (number_of - 1)
    while rest > 0:
        movable = [i for i in range(number_of - 1) if counts[i] < most]
        whole, left = sum([loads[i] for i in movable]), rest
        for i in movable:
            more = min(most - counts[i], max(1, left * loads[i] // whole), rest)
            counts[i] = counts[i] + more
            rest = rest - more
    return np.array([most] + counts)


def ragged(stream_key, count, total, reach, slope):
    if count == 2:
        one = jax.random.randint(stream_key, (), max(1, total - reach), min(reach, total - 1) + 1)
        return jnp.stack([one, total - one])
    sizes = jnp.asarray(split_up(count, total, reach, slope), jnp.int32)
    couples = (count - 1) // 2
    giver, sink = sizes[1:1 + 2 * couples:2], sizes[2:2 + 2 * couples:2]
    room = jnp.minimum(giver - 1, reach - sink)
    moved = jax.random.randint(jax.random.fold_in(stream_key, 1), (couples,), 0, 1 << 20) % (room + 1)
    sizes = sizes.at[1:1 + 2 * couples:2].set(giver - moved).at[2:2 + 2 * couples:2].set(sink + moved)
    return sizes[jax.random.permutation(jax.random.fold_in(stream_key, 2), count)]


def bell_draw(rng, dims, scale, most, shards=(), held_as=jnp.bfloat16):
    values = scale * jax.random.normal(rng, dims, jnp.float32)
    if shards:
        values = values * level_of(rng, dims, shards, -0.22, 0.18)
    return jnp.clip(values, -most, most).astype(held_as)


def gaussian_with(rng, dims, deviation, most, pieces, heavy, kind=jnp.bfloat16):
    array = deviation * jax.random.normal(rng, dims, jnp.float32)
    if pieces:
        array = array * level_of(rng, dims, pieces, -0.22, 0.18)
    return jnp.clip(strengthened(array, jax.random.fold_in(rng, 3), *heavy), -most, most).astype(kind)


def setup_inputs(seed: int = 0) -> dict:
    splits = jax.random.split(jax.random.key(seed), 21)
    hidden_rows = bell_draw(splits[0], (SEQS, D), 1.0, 6.0, ((1, 32),))
    first_gain = jnp.clip(1.0 + 0.18 * jax.random.normal(splits[1], (D,), jnp.float32), 0.1, 1.9)
    first_gate = gaussian_with(splits[2], (D, FF), D ** -0.5, 0.125, ((0, 8), (1, 4)), (0, 1, 8, 2.0))
    first_up = gaussian_with(splits[3], (D, FF), D ** -0.5, 0.125, ((0, 8), (1, 4)), (0, 1, 8, 2.0))
    first_down = gaussian_with(splits[4], (FF, D), FF ** -0.5, 0.078125, ((0, 4), (1, 8)), (0, 1, 8, 2.0))
    mix_gain = jnp.clip(1.0 + 0.18 * jax.random.normal(splits[5], (D,), jnp.float32), 0.1, 1.9)
    query_weight = bell_draw(splits[6], (D, HEADS * HEAD_DIM), D ** -0.5, 0.09375, ((0, 8), (1, 4)))
    key_weight = bell_draw(splits[7], (D, HEADS * HEAD_DIM), D ** -0.5, 0.09375, ((0, 8), (1, 4)))
    value_weight = bell_draw(splits[8], (D, HEADS * HEAD_DIM), D ** -0.5, 0.09375, ((0, 8), (1, 4)))
    forget_weight = bell_draw(splits[9], (D, HEADS), D ** -0.5, 0.09375, ((0, 8),))
    forget_bias = jnp.clip(jax.random.uniform(splits[10], (HEADS,), jnp.float32, -8.0, 2.0), -8.0, 2.0)
    out_weight = bell_draw(splits[11], (HEADS * HEAD_DIM, D), HEAD_DIM ** -0.5, 0.5, ((0, 4), (1, 8)))
    second_gain = jnp.clip(1.0 + 0.18 * jax.random.normal(splits[12], (D,), jnp.float32), 0.1, 1.9)
    second_gate = gaussian_with(splits[13], (D, FF), D ** -0.5, 0.125, ((0, 8), (1, 4)), (0, 1, 8, 2.0))
    second_up = gaussian_with(splits[14], (D, FF), D ** -0.5, 0.125, ((0, 8), (1, 4)), (0, 1, 8, 2.0))
    second_down = gaussian_with(splits[15], (FF, D), FF ** -0.5, 0.078125, ((0, 4), (1, 8)), (0, 1, 8, 2.0))
    cache_keys = draw_cache_keys(jax.random.fold_in(splits[20], 71), 0)
    cache_values = bell_draw(splits[17], (SEQS, LENGTH, HEADS * HEAD_DIM), 1.0, 6.0, ((1, 8), (2, 4)))
    cache_gates = draw_cache_gates(jax.random.fold_in(splits[20], 71), 0)
    lengths = ragged(splits[19], SEQS, SEQS * LENGTH // 4 + LENGTH, LENGTH, 2).astype(jnp.int32)
    return dict(hidden_rows=hidden_rows, first_gain=first_gain, first_gate=first_gate, first_up=first_up, first_down=first_down, mix_gain=mix_gain, query_weight=query_weight, key_weight=key_weight, value_weight=value_weight, forget_weight=forget_weight, forget_bias=forget_bias, out_weight=out_weight, second_gain=second_gain, second_gate=second_gate, second_up=second_up, second_down=second_down, cache_keys=cache_keys, cache_values=cache_values, cache_gates=cache_gates, lengths=lengths)


EPS = 1e-06
FLOOR = -1e+30

def half_block(rows, gain, w_gate, w_up, w_down):
    rows32 = rows.astype(jnp.float32)
    scaled = (rows32 * gain).astype(jnp.bfloat16)
    rscale = lax.rsqrt(lax.optimization_barrier(jnp.mean(rows32 * rows32, axis=1, keepdims=True)) + EPS)
    gate = jnp.dot(scaled, w_gate, preferred_element_type=jnp.float32) * rscale
    up_act = jnp.dot(scaled, w_up, preferred_element_type=jnp.float32) * rscale
    hidden = (jax.nn.silu(gate) * up_act).astype(jnp.bfloat16)
    down_sum = jnp.dot(hidden, w_down, preferred_element_type=jnp.float32)
    return (rows32 + 0.5 * down_sum).astype(jnp.bfloat16)

def mixing(rows, gain, query_weight, key_weight, value_weight, forget_weight, forget_bias, out_weight, cache_keys, cache_values, cache_gates, lengths):
    rows32 = rows.astype(jnp.float32)
    scaled = (rows32 * gain).astype(jnp.bfloat16)
    rscale = lax.rsqrt(lax.optimization_barrier(jnp.mean(rows32 * rows32, axis=1, keepdims=True)) + EPS)
    seqs = rows.shape[0]
    heads = forget_bias.shape[0]
    width = query_weight.shape[1]
    head_dim = width // heads
    query = lax.optimization_barrier((jnp.dot(scaled, query_weight, preferred_element_type=jnp.float32) * rscale).astype(jnp.bfloat16))
    fresh_key = lax.optimization_barrier((jnp.dot(scaled, key_weight, preferred_element_type=jnp.float32) * rscale).astype(jnp.bfloat16))
    fresh_value = lax.optimization_barrier((jnp.dot(scaled, value_weight, preferred_element_type=jnp.float32) * rscale).astype(jnp.bfloat16))
    fresh_gate = jax.nn.log_sigmoid(jnp.dot(scaled, forget_weight, preferred_element_type=jnp.float32) * rscale + forget_bias)
    query32 = query.astype(jnp.float32).reshape(seqs, heads, head_dim)
    key32 = fresh_key.astype(jnp.float32).reshape(seqs, heads, head_dim)
    value32 = fresh_value.astype(jnp.float32).reshape(seqs, heads, head_dim)
    total_len = cache_gates.shape[2]
    places = jnp.arange(total_len, dtype=jnp.int32)
    live = places[None, None, :] < lengths.astype(jnp.int32)[:, None, None]
    kept = jnp.where(live, cache_gates, 0.0)
    running = jnp.cumsum(kept, axis=2)
    bias = fresh_gate[:, :, None] + (running[:, :, -1:] - running)
    factor = head_dim ** (-0.5)
    span = POS_DEV
    blocks = total_len // span

    def step(carry, index):
        top_all, mass_all, summed_all = carry
        start = (index * span).astype(jnp.int32)
        keys = lax.dynamic_slice_in_dim(cache_keys, start, span, 1).astype(jnp.float32).reshape(seqs, span, heads, head_dim)
        values = lax.dynamic_slice_in_dim(cache_values, start, span, 1).astype(jnp.float32).reshape(seqs, span, heads, head_dim)
        bias_part = lax.dynamic_slice_in_dim(bias, start, span, 2)
        live_part = lax.dynamic_slice_in_dim(live, start, span, 2)
        scores = jnp.einsum('bphd,bhd->bhp', keys, query32) * factor + bias_part
        top = lax.optimization_barrier(jnp.max(jnp.where(live_part, scores, FLOOR), axis=2))
        weights = jnp.where(live_part, jnp.exp(scores - top[:, :, None]), 0.0)
        mass = lax.optimization_barrier(jnp.sum(weights, axis=2))
        rounded = lax.optimization_barrier(weights.astype(jnp.bfloat16)).astype(jnp.float32)
        summed = jnp.einsum('bhp,bphd->bhd', rounded, values)
        peak = jnp.maximum(top_all, top)
        old_part = jnp.exp(top_all - peak)
        new_part = jnp.exp(top - peak)
        return ((peak, mass_all * old_part + mass * new_part, summed_all * old_part[:, :, None] + summed * new_part[:, :, None]), None)
    start_carry = (jnp.full((seqs, heads), FLOOR, jnp.float32), jnp.zeros((seqs, heads), jnp.float32), jnp.zeros((seqs, heads, head_dim), jnp.float32))
    (top, mass, summed), _ = lax.scan(step, start_carry, jnp.arange(blocks, dtype=jnp.int32))
    own = lax.optimization_barrier(jnp.sum(query32 * key32, axis=2)) * factor
    peak = jnp.maximum(top, own)
    keep = jnp.exp(top - peak)
    fresh = jnp.exp(own - peak)
    attended = ((summed * keep[:, :, None] + value32 * fresh[:, :, None]) / (mass * keep + fresh)[:, :, None]).astype(jnp.bfloat16).reshape(seqs, width)
    mixed = jnp.dot(attended, out_weight, preferred_element_type=jnp.float32)
    return (rows32 + mixed).astype(jnp.bfloat16)

def reference(hidden_rows, first_gain, first_gate, first_up, first_down, mix_gain, query_weight, key_weight, value_weight, forget_weight, forget_bias, out_weight, second_gain, second_gate, second_up, second_down, cache_keys, cache_values, cache_gates, lengths):
    mid_rows = half_block(hidden_rows, first_gain, first_gate, first_up, first_down)
    after_rows = mixing(mid_rows, mix_gain, query_weight, key_weight, value_weight, forget_weight, forget_bias, out_weight, cache_keys, cache_values, cache_gates, lengths)
    return half_block(after_rows, second_gain, second_gate, second_up, second_down)
```

```python
import functools

import jax
import jax.numpy as jnp
from jax import lax
from jax.experimental import pallas as pl
from jax.experimental.pallas import tpu as pltpu
from jax.sharding import PartitionSpec as P

HEAD_DIM = 128
LANES = 128
SUB = 8
EPS = 1e-06
FLOOR = -1e30
MESH = pl.DeviceIdType.MESH
F32 = jnp.float32
BF16 = jnp.bfloat16

RS1, AG1, RSQ, AGQ, RSA, AGA, RS2, AG2 = range(8)
GATHER, SUM1, SUM2, SUM3 = range(4)


def up_to(value, step):
    return -(-value // step) * step


def hi_lo(column, rows):
    lane = lax.broadcasted_iota(jnp.int32, (rows, LANES), 1)
    wide = jnp.broadcast_to(column, (rows, LANES))
    hi = wide.astype(BF16).astype(F32)
    return jnp.where(lane < LANES // 2, hi, wide - hi).astype(BF16)


def from_hi_lo(tile):
    return tile[:, 0:1] + tile[:, LANES // 2 : LANES // 2 + 1]


def dot(a, b):
    return jnp.dot(a, b, preferred_element_type=F32)


def kernel(
    c,
    hid, g1, gm, g2, fw, cg, fb, lens,
    wg1, wu1, wd1, wq, wk, wv, wo, wg2, wu2, wd2, ck, cv,
    out,
    wg1_v, wu1_v, wd1_v, wq_v, wk_v, wv_v, wo_v, wg2_v, wu2_v, wd2_v, ck_v, cv_v,
    xg, rs_send1, rs_recv1, hid1, sum1_send, sum1,
    q_send, q_recv, q_buf, q_all, fwx, gpad, bias, total, sc, pv, stat, a_send, a_recv, att, att_all,
    sum2_send, sum2, rs_send2, rs_recv2, hid2, fin_send, fin_recv, fin_x, rows,
    ld_sem, kv_send, kv_recv, tp_send, tp_recv,
):
    K, T, R, RP = c["K"], c["T"], c["R"], c["RP"]
    ff, CW, nown, heads, span, width = c["ff"], c["CW"], c["nown"], c["heads"], c["span"], c["width"]
    NC = heads * (RP // 16)
    halves = RP // 16
    features = c["features"]
    me = lax.axis_index("kv")
    mt = lax.axis_index("tp")

    sends = []

    def guarded(limit, who, fn):
        if limit >= K:
            fn()
        else:
            pl.when(who < limit)(fn)

    def kv_copy(phase, src, dst, j):
        return pltpu.make_async_remote_copy(
            src_ref=src, dst_ref=dst, send_sem=kv_send.at[phase, j], recv_sem=kv_recv.at[phase, me],
            device_id={"kv": j}, device_id_type=MESH)

    def kv_wait(phase, dst, s):
        pltpu.make_async_remote_copy(
            src_ref=dst, dst_ref=dst, send_sem=kv_send.at[phase, s], recv_sem=kv_recv.at[phase, s],
            device_id={"kv": s}, device_id_type=MESH).wait_recv()

    def tp_copy(phase, src, dst, j):
        return pltpu.make_async_remote_copy(
            src_ref=src, dst_ref=dst, send_sem=tp_send.at[phase, j], recv_sem=tp_recv.at[phase, mt],
            device_id={"tp": j}, device_id_type=MESH)

    def tp_wait(phase, dst, s):
        pltpu.make_async_remote_copy(
            src_ref=dst, dst_ref=dst, send_sem=tp_send.at[phase, s], recv_sem=tp_recv.at[phase, s],
            device_id={"tp": s}, device_id_type=MESH).wait_recv()

    def kv_peer(i):
        return lax.rem(me + i, K)

    def tp_peer(i):
        return lax.rem(mt + i, T)

    count = [0]

    def load(src, dst):
        cp = pltpu.make_async_copy(src, dst, ld_sem.at[count[0]])
        count[0] += 1
        cp.start()
        return cp

    def load_cols(src, dst):
        n = src.shape[0]
        step = n // 4 if n % 64 == 0 else n
        return [load(src.at[pl.ds(r, step), :], dst.at[pl.ds(r, step), pl.ds(0, ff)]) for r in range(0, n, step)]

    def load_rows(src, dst):
        step = ff // 2 if ff % 32 == 0 else ff
        return [load(src.at[pl.ds(r, step), :], dst.at[pl.ds(r, step), :]) for r in range(0, ff, step)]

    def load_seqs(src, dst):
        step = 7 if R % 7 == 0 else R
        return [load(src.at[pl.ds(r, step)], dst.at[pl.ds(r, step)]) for r in range(0, R, step)]

    def wait_all(cps):
        for cp in cps:
            cp.wait()

    in1 = load_cols(wg1, wg1_v) + load_cols(wu1, wu1_v)

    barrier = pltpu.get_barrier_semaphore()
    for i in range(1, K):
        pl.semaphore_signal(barrier, inc=1, device_id={"kv": kv_peer(i)}, device_id_type=MESH)
    for i in range(1, T):
        pl.semaphore_signal(barrier, inc=1, device_id={"tp": tp_peer(i)}, device_id_type=MESH)

    down1 = load_rows(wd1, wd1_v)

    if nown * CW > ff:
        for w in (wg1_v, wu1_v, wg2_v, wu2_v):
            w[:, ff:] = jnp.zeros((w.shape[0], nown * CW - ff), BF16)
        for w in (wd1_v, wd2_v):
            w[ff:, :] = jnp.zeros((nown * CW - ff, w.shape[1]), BF16)

    xg_pad = jnp.zeros((RP - R, hid.shape[1]), BF16)
    xg[mt] = jnp.concatenate([hid[...], xg_pad], axis=0)

    pl.semaphore_wait(barrier, K - 1 + T - 1)

    if c["gathered"]:
        x = xg[mt]
    else:
        for i in range(1, T):
            cp = tp_copy(GATHER, xg.at[mt], xg.at[mt], tp_peer(i))
            cp.start()
            sends.append((None, None, cp))

    slot_all = c["head_total"]
    pick_row = lax.broadcasted_iota(jnp.int32, (slot_all, width), 0)
    pick_head = mt * heads + lax.broadcasted_iota(jnp.int32, (slot_all, width), 1) // HEAD_DIM
    fwx[...] = dot(fw[...], jnp.where(pick_row == pick_head, 1.0, 0.0).astype(BF16)).astype(BF16)

    place = me * span + lax.broadcasted_iota(jnp.int32, (SUB, span), 1)
    gpad[...] = jnp.zeros_like(gpad)
    for b in range(R):
        live = place[0:heads] < lens[b]
        gpad[b * SUB : b * SUB + heads, :] = jnp.where(live, cg[b], 0.0)
    kept = gpad[...]
    later = jnp.where(
        lax.broadcasted_iota(jnp.int32, (span, span), 0) > lax.broadcasted_iota(jnp.int32, (span, span), 1), 1.0, 0.0
    ).astype(BF16)
    top16 = kept.astype(BF16)
    rest = kept - top16.astype(F32)
    mid16 = rest.astype(BF16)
    low16 = (rest - mid16.astype(F32)).astype(BF16)
    after = dot(top16, later) + dot(mid16, later) + dot(low16, later)
    bias[...] = after
    total[...] = jnp.broadcast_to(after[:, 0:1] + kept[:, 0:1], total.shape)
    sc[...] = jnp.full_like(sc, FLOOR)
    pv[...] = jnp.zeros_like(pv)

    if not c["gathered"]:
        for i in range(1, T):
            tp_wait(GATHER, xg.at[tp_peer(i)], tp_peer(i))
        x = jnp.concatenate([xg[t] for t in range(T)], axis=1)

    def scaled_rows(x, gain):
        x32 = x.astype(F32)
        return (x32 * gain[...]).astype(BF16), jnp.sum(x32 * x32, axis=1, keepdims=True)

    def feed_forward(x, gain, loads, wg_v, wu_v, down, wd_v, rs_send, rs_recv, hbuf, rs, ag, extra):
        scaled, squares = scaled_rows(x, gain)
        square_tile = hi_lo(squares, RP)
        wait_all(loads)

        def part(j, dst):
            cols = pl.ds(pl.multiple_of(j * CW, LANES), CW)
            dst[:, 0:CW] = dot(scaled, wg_v[:, cols]).astype(BF16)
            dst[:, CW : 2 * CW] = dot(scaled, wu_v[:, cols]).astype(BF16)
            dst[:, 2 * CW :] = square_tile

        for i in range(1, K):
            j = kv_peer(i)

            def one(j=j):
                part(j, rs_send.at[j])
                kv_copy(rs, rs_send.at[j], rs_recv.at[me], j).start()

            guarded(nown, j, one)
            sends.append((nown, j, kv_copy(rs, rs_send.at[j], rs_recv.at[me], j)))

        guarded(nown, me, lambda: part(me, rs_recv.at[me]))
        more = extra()

        def own():
            tot = rs_recv[me].astype(F32)
            for i in range(1, K):
                s = kv_peer(i)
                kv_wait(rs, rs_recv.at[s], s)
                tot = tot + rs_recv[s].astype(F32)
            rscale = lax.rsqrt(from_hi_lo(tot[:, 2 * CW :]) / features + EPS)
            gate = tot[:, 0:CW] * rscale
            hbuf[me] = (gate / (1.0 + jnp.exp(-gate)) * (tot[:, CW : 2 * CW] * rscale)).astype(BF16)
            for i in range(1, K):
                kv_copy(ag, hbuf.at[me], hbuf.at[me], kv_peer(i)).start()

        guarded(nown, me, own)
        for i in range(1, K):
            sends.append((nown, me, kv_copy(ag, hbuf.at[me], hbuf.at[me], kv_peer(i))))
        wait_all(down)
        if nown == K:
            acc = dot(hbuf[me], wd_v[pl.ds(pl.multiple_of(me * CW, LANES), CW), :])
            for i in range(1, K):
                s = kv_peer(i)
                kv_wait(ag, hbuf.at[s], s)
                acc = acc + dot(hbuf[s], wd_v[pl.ds(pl.multiple_of(s * CW, LANES), CW), :])
        else:
            acc = jnp.zeros((RP, wd_v.shape[1]), F32)
            for s in range(nown):
                pl.when(me != s)(functools.partial(kv_wait, ag, hbuf.at[s], s))
                acc = acc + dot(hbuf[s], wd_v[s * CW : (s + 1) * CW, :])
        return acc, more

    def tp_sum(phase, acc, send, buf):
        send[...] = acc.astype(BF16)
        for i in range(1, T):
            cp = tp_copy(phase, send, buf.at[mt], tp_peer(i))
            cp.start()
            sends.append((None, None, cp))
        buf[mt] = send[...]
        for i in range(1, T):
            tp_wait(phase, buf.at[tp_peer(i)], tp_peer(i))
        tot = buf[0].astype(F32)
        for t in range(1, T):
            tot = tot + buf[t].astype(F32)
        return tot

    def rest_of_loads():
        proj = [load(wq, wq_v), load(wk, wk_v), load(wv, wv_v)]
        keys = load_seqs(ck, ck_v)
        values = load_seqs(cv, cv_v)
        proj_out = [load(wo, wo_v)]
        in2 = load_cols(wg2, wg2_v) + load_cols(wu2, wu2_v)
        down2 = load_rows(wd2, wd2_v)
        return proj, keys, values, proj_out, in2, down2

    acc, (proj, keys, values, proj_out, in2, down2) = feed_forward(
        x, g1, in1, wg1_v, wu1_v, down1, wd1_v, rs_send1, rs_recv1, hid1, RS1, AG1, rest_of_loads)
    x = (x.astype(F32) + 0.5 * tp_sum(SUM1, acc, sum1_send, sum1)).astype(BF16)

    scaled, squares = scaled_rows(x, gm)
    wait_all(proj)
    pq, pk, pvv, plog = dot(scaled, wq_v[...]), dot(scaled, wk_v[...]), dot(scaled, wv_v[...]), dot(scaled, fwx[...])
    square_tile = hi_lo(squares, RP)
    for n in range(NC):
        h, half = n // halves, n % halves
        r, l = slice(half * 16, half * 16 + 16), slice(h * HEAD_DIM, (h + 1) * HEAD_DIM)
        q_send[n, 0] = pq[r, l].astype(BF16)
        q_send[n, 1] = pk[r, l].astype(BF16)
        q_send[n, 2] = pvv[r, l].astype(BF16)
        q_send[n, 3] = hi_lo(plog[r, h * HEAD_DIM : h * HEAD_DIM + 1], 16)
        q_send[n, 4] = square_tile[r]

    def to_owners(phase, send, recv):
        for i in range(1, K):
            j = kv_peer(i)
            cp = kv_copy(phase, send.at[j], recv.at[me], j)
            guarded(NC, j, cp.start)
            sends.append((NC, j, cp))

    def gather_chunks(phase, buf):
        for n in range(NC):
            pl.when(me != n)(functools.partial(kv_wait, phase, buf.at[n], n))

    to_owners(RSQ, q_send, q_recv)
    factor = HEAD_DIM ** (-0.5)
    my_head = mt * heads + lax.rem(me, NC) // halves
    mine = lax.rem(me, NC)

    def own_query():
        q_recv[me] = q_send[mine]
        tot = [q_recv[me, p].astype(F32) for p in range(5)]
        for i in range(1, K):
            s = kv_peer(i)
            kv_wait(RSQ, q_recv.at[s], s)
            tot = [t + q_recv[s, p].astype(F32) for p, t in enumerate(tot)]
        rscale = lax.rsqrt(from_hi_lo(tot[4]) / features + EPS)
        query = (tot[0] * rscale).astype(BF16)
        q_buf[mine] = query
        for i in range(1, K):
            kv_copy(AGQ, q_buf.at[mine], q_buf.at[mine], kv_peer(i)).start()
        q32 = query.astype(F32)
        k32 = (tot[1] * rscale).astype(BF16).astype(F32)
        v32 = (tot[2] * rscale).astype(BF16).astype(F32)
        logit = from_hi_lo(tot[3]) * rscale + fb[my_head]
        rows[0] = jnp.broadcast_to(jnp.sum(q32 * k32, axis=1, keepdims=True) * factor, (16, LANES))
        rows[1] = v32
        rows[2] = jnp.broadcast_to(
            jnp.minimum(logit, 0.0) - jnp.log(1.0 + jnp.exp(-jnp.abs(logit))), (16, LANES))

    guarded(NC, me, own_query)
    for i in range(1, K):
        sends.append((NC, me, kv_copy(AGQ, q_buf.at[mine], q_buf.at[mine], kv_peer(i))))
    wait_all(keys)
    gather_chunks(AGQ, q_buf)
    for n in range(NC):
        h, half = n // halves, n % halves
        q_all[half * 16 : half * 16 + 16, h * HEAD_DIM : (h + 1) * HEAD_DIM] = q_buf[n].astype(F32)

    sel = lax.broadcasted_iota(jnp.int32, (SUB, width), 0) == lax.broadcasted_iota(jnp.int32, (SUB, width), 1) // HEAD_DIM
    for b in range(R):
        qb = jnp.where(sel, jnp.broadcast_to(q_all[b : b + 1, :], (SUB, width)), 0.0).astype(BF16)
        s = lax.dot_general(qb, ck_v[b], (((1,), (1,)), ((), ())), preferred_element_type=F32)
        s = s * factor + bias[b * SUB : (b + 1) * SUB, :]
        sc[b * SUB : (b + 1) * SUB, :] = jnp.where(place < lens[b], s, FLOOR)
    s = sc[...]
    top = jnp.max(s, axis=1, keepdims=True)
    weights = jnp.where(s > 0.5 * FLOOR, jnp.exp(s - top), 0.0)
    mass = jnp.sum(weights, axis=1, keepdims=True)
    sc[...] = weights
    lane = lax.broadcasted_iota(jnp.int32, stat.shape, 1)
    stat[...] = jnp.where(lane < 32, top, jnp.where(lane < 64, mass, total[...]))
    wait_all(values)
    for b in range(R):
        part = dot(sc[b * SUB : (b + 1) * SUB, :].astype(BF16), cv_v[b])
        for h in range(heads):
            pv[h, b * SUB : (b + 1) * SUB, :] = part[:, h * HEAD_DIM : (h + 1) * HEAD_DIM]
    for n in range(NC):
        h, half = n // halves, n % halves
        picked = pl.ds(half * 16 * SUB + h, 16, stride=SUB)
        a_send[n, 0] = pv.at[h][picked, :]
        a_send[n, 1] = stat[picked, :]

    to_owners(RSA, a_send, a_recv)

    def own_attended():
        a_recv[me] = a_send[mine]
        for i in range(1, K):
            kv_wait(RSA, a_recv.at[kv_peer(i)], kv_peer(i))
        own_score, fresh_value, fresh_gate = rows[0], rows[1], rows[2]
        ahead = fresh_gate
        tops = [None] * K
        for s in reversed(range(K)):
            st = a_recv[s, 1]
            tops[s] = st[:, 0:1] + ahead
            ahead = ahead + st[:, 64:65]
        peak = own_score
        for s in range(K):
            peak = jnp.maximum(peak, tops[s])
        fresh = jnp.exp(own_score - peak)
        num, den = fresh * fresh_value, fresh
        for s in range(K):
            keep = jnp.exp(tops[s] - peak)
            num = num + keep * a_recv[s, 0]
            den = den + keep * a_recv[s, 1][:, 32:33]
        att[mine] = (num / den).astype(BF16)
        for i in range(1, K):
            kv_copy(AGA, att.at[mine], att.at[mine], kv_peer(i)).start()

    guarded(NC, me, own_attended)
    for i in range(1, K):
        sends.append((NC, me, kv_copy(AGA, att.at[mine], att.at[mine], kv_peer(i))))
    wait_all(proj_out)
    gather_chunks(AGA, att)
    for n in range(NC):
        h, half = n // halves, n % halves
        att_all[half * 16 : half * 16 + 16, h * HEAD_DIM : (h + 1) * HEAD_DIM] = att[n]
    acc = dot(att_all[...], wo_v[...])
    x = (x.astype(F32) + tp_sum(SUM2, acc, sum2_send, sum2)).astype(BF16)

    acc, _ = feed_forward(
        x, g2, in2, wg2_v, wu2_v, down2, wd2_v, rs_send2, rs_recv2, hid2, RS2, AG2, lambda: None)

    if c["gathered"]:
        tot = tp_sum(SUM3, acc, fin_send, fin_recv)
        out[...] = (x.astype(F32) + 0.5 * tot).astype(BF16)[0:R]
    else:
        cols = hid.shape[1]
        for t in range(T):
            fin_send[t] = acc[:, t * cols : (t + 1) * cols]
            fin_x[t] = x[:, t * cols : (t + 1) * cols]
        for i in range(1, T):
            cp = tp_copy(SUM3, fin_send.at[tp_peer(i)], fin_recv.at[mt], tp_peer(i))
            cp.start()
            sends.append((None, None, cp))
        fin_recv[mt] = fin_send[mt]
        for i in range(1, T):
            tp_wait(SUM3, fin_recv.at[tp_peer(i)], tp_peer(i))
        tot = fin_recv[0]
        for t in range(1, T):
            tot = tot + fin_recv[t]
        out[...] = (fin_x[mt].astype(F32) + 0.5 * tot).astype(BF16)[0:R]

    for limit, who, cp in sends:
        if limit is None:
            cp.wait_send()
        else:
            guarded(limit, who, cp.wait_send)


def local(
    K, T,
    hidden_rows, first_gain, first_gate, first_up, first_down, mix_gain,
    query_weight, key_weight, value_weight, forget_weight, forget_bias, out_weight,
    second_gain, second_gate, second_up, second_down,
    cache_keys, cache_values, cache_gates, lengths,
):
    R, cols = hidden_rows.shape
    Dl = first_gate.shape[0]
    gathered = cols % LANES != 0
    RP = up_to(R, 16)
    width = query_weight.shape[1]
    heads = width // HEAD_DIM
    span = cache_keys.shape[1]
    ff = up_to(first_gate.shape[1], LANES)
    short = ff - first_gate.shape[1]
    if short:
        first_gate, first_up, second_gate, second_up = (
            jnp.pad(w, ((0, 0), (0, short))) for w in (first_gate, first_up, second_gate, second_up))
        first_down, second_down = (jnp.pad(w, ((0, short), (0, 0))) for w in (first_down, second_down))
    tiles = ff // LANES
    CW = up_to(tiles, K) // K * LANES
    nown = -(-ff // CW)
    ffc = nown * CW
    NC = heads * (RP // 16)
    assert NC <= K and heads <= SUB
    rows_in = lax.all_gather(hidden_rows, "tp", axis=1, tiled=True) if gathered else hidden_rows
    c = dict(K=K, T=T, R=R, RP=RP, ff=ff, CW=CW, nown=nown, heads=heads, span=span, width=width,
             features=Dl * K, gathered=gathered, head_total=forget_bias.shape[0])
    xc = rows_in.shape[1]
    vm = pltpu.VMEM
    msg = 2 * CW + LANES
    scratch = [
        vm((Dl, ffc), BF16), vm((Dl, ffc), BF16), vm((ffc, Dl), BF16),
        vm((Dl, width), BF16), vm((Dl, width), BF16), vm((Dl, width), BF16), vm((width, Dl), BF16),
        vm((Dl, ffc), BF16), vm((Dl, ffc), BF16), vm((ffc, Dl), BF16),
        vm((R, span, width), BF16), vm((R, span, width), BF16),
        vm((T, RP, xc), BF16), vm((K, RP, msg), BF16), vm((K, RP, msg), BF16), vm((K, RP, CW), BF16),
        vm((RP, Dl), BF16), vm((T, RP, Dl), BF16),
        vm((K, 5, 16, LANES), BF16), vm((K, 5, 16, LANES), BF16), vm((NC, 16, LANES), BF16), vm((RP, width), F32),
        vm((Dl, width), BF16), vm((RP * SUB, span), F32), vm((RP * SUB, span), F32), vm((RP * SUB, LANES), F32),
        vm((RP * SUB, span), F32), vm((heads, RP * SUB, LANES), F32), vm((RP * SUB, LANES), F32),
        vm((K, 2, 16, LANES), F32), vm((K, 2, 16, LANES), F32), vm((NC, 16, LANES), BF16), vm((RP, width), BF16),
        vm((RP, Dl), BF16), vm((T, RP, Dl), BF16),
        vm((K, RP, msg), BF16), vm((K, RP, msg), BF16), vm((K, RP, CW), BF16),
        vm((RP, Dl), BF16) if gathered else vm((T, RP, xc), F32),
        vm((T, RP, Dl), BF16) if gathered else vm((T, RP, xc), F32),
        vm((T, RP, xc), BF16), vm((3, 16, LANES), F32),
        pltpu.SemaphoreType.DMA((48,)),
        pltpu.SemaphoreType.DMA((8, K)), pltpu.SemaphoreType.DMA((8, K)),
        pltpu.SemaphoreType.DMA((4, T)), pltpu.SemaphoreType.DMA((4, T)),
    ]
    in_vmem = pl.BlockSpec(memory_space=pltpu.VMEM)
    in_smem = pl.BlockSpec(memory_space=pltpu.SMEM)
    anywhere = pl.BlockSpec(memory_space=pl.ANY)
    result = pl.pallas_call(
        functools.partial(kernel, c),
        out_shape=jax.ShapeDtypeStruct((R, xc), BF16),
        in_specs=[in_vmem] * 6 + [in_smem] * 2 + [anywhere] * 12,
        out_specs=in_vmem,
        scratch_shapes=scratch,
        compiler_params=pltpu.CompilerParams(
            collective_id=0, has_side_effects=True, vmem_limit_bytes=60 * 1024 * 1024),
        name="layer",
    )(
        rows_in, first_gain.reshape(1, Dl), mix_gain.reshape(1, Dl), second_gain.reshape(1, Dl),
        forget_weight, cache_gates, forget_bias, lengths,
        first_gate, first_up, first_down, query_weight, key_weight, value_weight, out_weight,
        second_gate, second_up, second_down, cache_keys, cache_values,
    )
    if gathered:
        return lax.dynamic_slice_in_dim(result, lax.axis_index("tp") * cols, cols, 1)
    return result


def solution(mesh):
    return jax.shard_map(
        functools.partial(local, mesh.shape["kv"], mesh.shape["tp"]),
        mesh=mesh,
        in_specs=(
            P(None, ("kv", "tp")),
            P("kv"),
            P("kv", "tp"),
            P("kv", "tp"),
            P("tp", "kv"),
            P("kv"),
            P("kv", "tp"),
            P("kv", "tp"),
            P("kv", "tp"),
            P("kv", None),
            P(),
            P("tp", "kv"),
            P("kv"),
            P("kv", "tp"),
            P("kv", "tp"),
            P("tp", "kv"),
            P(None, "kv", "tp"),
            P(None, "kv", "tp"),
            P(None, "tp", "kv"),
            P(),
        ),
        out_specs=P(None, ("kv", "tp")),
        check_vma=False,
    )
```

```python
import functools

import jax
import jax.numpy as jnp
from jax import lax
from jax.experimental import pallas as pl
from jax.experimental.pallas import tpu as pltpu
from jax.sharding import PartitionSpec as P

HEAD_DIM = 128
LANES = 128
SUB = 8
EPS = 1e-06
FLOOR = -1e30
MESH = pl.DeviceIdType.MESH
F32 = jnp.float32
BF16 = jnp.bfloat16

RS1, AG1, RSQ, AGQ, RSA, AGA, RS2, AG2, SQ1, SQM, SQ2, RSK, RSS = range(13)
GATHER, SUM1, SUM2, SUM3 = range(4)


def up_to(value, step):
    return -(-value // step) * step


def hi_lo(column, rows):
    lane = lax.broadcasted_iota(jnp.int32, (rows, LANES), 1)
    wide = jnp.broadcast_to(column, (rows, LANES))
    hi = wide.astype(BF16).astype(F32)
    return jnp.where(lane < LANES // 2, hi, wide - hi).astype(BF16)


def from_hi_lo(tile):
    return tile[:, 0:1] + tile[:, LANES // 2 : LANES // 2 + 1]


def pack_column(column, parts):
    lane = lax.broadcasted_iota(jnp.int32, (SUB, LANES), 1) // (LANES // parts)
    tile = jnp.broadcast_to(column[0:SUB], (SUB, LANES))
    for p in range(1, parts):
        tile = jnp.where(lane == p, column[p * SUB : (p + 1) * SUB], tile)
    return tile


def unpack_column(tile, parts, offset=0):
    step = LANES // parts
    return jnp.concatenate([tile[:, p * step + offset : p * step + offset + 1] for p in range(parts)], axis=0)


def dot(a, b):
    return jnp.dot(a, b, preferred_element_type=F32)


def kernel(
    c,
    hid, g1, gm, g2, fw, cg, fb, lens,
    wg1, wu1, wd1, wq, wk, wv, wo, wg2, wu2, wd2, ck, cv,
    out,
    wg1_v, wu1_v, wd1_v, wq_v, wk_v, wv_v, wo_v, wg2_v, wu2_v, wd2_v, ck_v, cv_v,
    xg, rs_send1, rs_recv1, hid1, sum1_send, sum1,
    sq_send, sq_recv, q_send, q_recv, k_send, k_recv, q_buf, q_all, fwx, gpad, bias, total, sc, pv, stat, a_send, a_recv, s_send, s_recv, att, att_all,
    sum2_send, sum2, rs_send2, rs_recv2, hid2, fin_send, fin_recv, fin_x, rows,
    ld_sem, kv_send, kv_recv, tp_send, tp_recv,
):
    K, T, R, RP = c["K"], c["T"], c["R"], c["RP"]
    ff, CW, nown, heads, span, width = c["ff"], c["CW"], c["nown"], c["heads"], c["span"], c["width"]
    NC = heads * (RP // 16)
    halves = RP // 16
    features = c["features"]
    me = lax.axis_index("kv")
    mt = lax.axis_index("tp")

    sends = []

    def guarded(limit, who, fn):
        if limit >= K:
            fn()
        else:
            pl.when(who < limit)(fn)

    def kv_copy(phase, src, dst, j):
        return pltpu.make_async_remote_copy(
            src_ref=src, dst_ref=dst, send_sem=kv_send.at[phase, j], recv_sem=kv_recv.at[phase, me],
            device_id={"kv": j}, device_id_type=MESH)

    def kv_wait(phase, dst, s):
        pltpu.make_async_remote_copy(
            src_ref=dst, dst_ref=dst, send_sem=kv_send.at[phase, s], recv_sem=kv_recv.at[phase, s],
            device_id={"kv": s}, device_id_type=MESH).wait_recv()

    def tp_copy(phase, src, dst, j):
        return pltpu.make_async_remote_copy(
            src_ref=src, dst_ref=dst, send_sem=tp_send.at[phase, j], recv_sem=tp_recv.at[phase, mt],
            device_id={"tp": j}, device_id_type=MESH)

    def tp_wait(phase, dst, s):
        pltpu.make_async_remote_copy(
            src_ref=dst, dst_ref=dst, send_sem=tp_send.at[phase, s], recv_sem=tp_recv.at[phase, s],
            device_id={"tp": s}, device_id_type=MESH).wait_recv()

    def kv_peer(i):
        return lax.rem(me + i, K)

    def tp_peer(i):
        return lax.rem(mt + i, T)

    count = [0]

    def load(src, dst):
        cp = pltpu.make_async_copy(src, dst, ld_sem.at[count[0]])
        count[0] += 1
        cp.start()
        return cp

    def load_cols(src, dst):
        n = src.shape[0]
        step = n // 4 if n % 64 == 0 else n
        return [load(src.at[pl.ds(r, step), :], dst.at[pl.ds(r, step), pl.ds(0, ff)]) for r in range(0, n, step)]

    def load_rows(src, dst):
        step = ff // 2 if ff % 32 == 0 else ff
        return [load(src.at[pl.ds(r, step), :], dst.at[pl.ds(r, step), :]) for r in range(0, ff, step)]

    def load_seqs(src, dst):
        step = 7 if R % 7 == 0 else R
        return [load(src.at[pl.ds(r, step)], dst.at[pl.ds(r, step)]) for r in range(0, R, step)]

    def wait_all(cps):
        for cp in cps:
            cp.wait()

    in1 = load_cols(wg1, wg1_v) + load_cols(wu1, wu1_v)

    barrier = pltpu.get_barrier_semaphore()
    for i in range(1, K):
        pl.semaphore_signal(barrier, inc=1, device_id={"kv": kv_peer(i)}, device_id_type=MESH)
    for i in range(1, T):
        pl.semaphore_signal(barrier, inc=1, device_id={"tp": tp_peer(i)}, device_id_type=MESH)

    down1 = load_rows(wd1, wd1_v)

    if nown * CW > ff:
        for w in (wg1_v, wu1_v, wg2_v, wu2_v):
            w[:, ff:] = jnp.zeros((w.shape[0], nown * CW - ff), BF16)
        for w in (wd1_v, wd2_v):
            w[ff:, :] = jnp.zeros((nown * CW - ff, w.shape[1]), BF16)

    xg_pad = jnp.zeros((RP - R, hid.shape[1]), BF16)
    xg[mt] = jnp.concatenate([hid[...], xg_pad], axis=0)

    pl.semaphore_wait(barrier, K - 1 + T - 1)

    if c["gathered"]:
        x = xg[mt]
    else:
        for i in range(1, T):
            cp = tp_copy(GATHER, xg.at[mt], xg.at[mt], tp_peer(i))
            cp.start()
            sends.append((None, None, cp))

    slot_all = c["head_total"]
    pick_row = lax.broadcasted_iota(jnp.int32, (slot_all, width), 0)
    pick_head = mt * heads + lax.broadcasted_iota(jnp.int32, (slot_all, width), 1) // HEAD_DIM
    fwx[...] = dot(fw[...], jnp.where(pick_row == pick_head, 1.0, 0.0).astype(BF16)).astype(BF16)

    place = me * span + lax.broadcasted_iota(jnp.int32, (SUB, span), 1)
    gpad[...] = jnp.zeros_like(gpad)
    for b in range(R):
        live = place[0:heads] < lens[b]
        gpad[b * SUB : b * SUB + heads, :] = jnp.where(live, cg[b], 0.0)
    kept = gpad[...]
    later = jnp.where(
        lax.broadcasted_iota(jnp.int32, (span, span), 0) > lax.broadcasted_iota(jnp.int32, (span, span), 1), 1.0, 0.0
    ).astype(BF16)
    top16 = kept.astype(BF16)
    rest = kept - top16.astype(F32)
    mid16 = rest.astype(BF16)
    low16 = (rest - mid16.astype(F32)).astype(BF16)
    after = dot(top16, later) + dot(mid16, later) + dot(low16, later)
    bias[...] = after
    total[...] = jnp.broadcast_to(after[:, 0:1] + kept[:, 0:1], total.shape)
    sc[...] = jnp.full_like(sc, FLOOR)
    pv[...] = jnp.zeros_like(pv)

    if not c["gathered"]:
        for i in range(1, T):
            tp_wait(GATHER, xg.at[tp_peer(i)], tp_peer(i))
        x = jnp.concatenate([xg[t] for t in range(T)], axis=1)

    def scaled_rows(x, gain):
        x32 = x.astype(F32)
        return (x32 * gain[...]).astype(BF16), jnp.sum(x32 * x32, axis=1, keepdims=True)

    parts = RP // SUB

    def send_squares(n, phase, squares, limit):
        sq_send[n] = pack_column(squares, parts)
        for i in range(1, K):
            j = kv_peer(i)
            cp = kv_copy(phase, sq_send.at[n], sq_recv.at[n, me], j)
            guarded(limit, j, cp.start)
            sends.append((limit, j, cp))
        sq_recv[n, me] = sq_send[n]

    def row_scale(n, phase):
        tot = sq_recv[n, me]
        for i in range(1, K):
            s = kv_peer(i)
            kv_wait(phase, sq_recv.at[n, s], s)
            tot = tot + sq_recv[n, s]
        return lax.rsqrt(unpack_column(tot, parts) / features + EPS)

    def feed_forward(n, sq, x, gain, loads, wg_v, wu_v, down, wd_v, rs_send, rs_recv, hbuf, rs, ag, extra):
        scaled, squares = scaled_rows(x, gain)
        send_squares(n, sq, squares, nown)
        wait_all(loads)

        def part(j, dst):
            cols = pl.ds(pl.multiple_of(j * CW, LANES), CW)
            dst[:, 0:CW] = dot(scaled, wg_v[:, cols]).astype(BF16)
            dst[:, CW : 2 * CW] = dot(scaled, wu_v[:, cols]).astype(BF16)

        for i in range(1, K):
            j = kv_peer(i)

            def one(j=j):
                part(j, rs_send.at[j])
                kv_copy(rs, rs_send.at[j], rs_recv.at[me], j).start()

            guarded(nown, j, one)
            sends.append((nown, j, kv_copy(rs, rs_send.at[j], rs_recv.at[me], j)))

        guarded(nown, me, lambda: part(me, rs_recv.at[me]))
        more = extra()

        def own():
            rscale = row_scale(n, sq)
            tot = rs_recv[me].astype(F32)
            for i in range(1, K):
                s = kv_peer(i)
                kv_wait(rs, rs_recv.at[s], s)
                tot = tot + rs_recv[s].astype(F32)
            gate = tot[:, 0:CW] * rscale
            hbuf[me] = (gate / (1.0 + jnp.exp(-gate)) * (tot[:, CW : 2 * CW] * rscale)).astype(BF16)
            for i in range(1, K):
                kv_copy(ag, hbuf.at[me], hbuf.at[me], kv_peer(i)).start()

        guarded(nown, me, own)
        for i in range(1, K):
            sends.append((nown, me, kv_copy(ag, hbuf.at[me], hbuf.at[me], kv_peer(i))))
        wait_all(down)
        if nown == K:
            acc = dot(hbuf[me], wd_v[pl.ds(pl.multiple_of(me * CW, LANES), CW), :])
            for i in range(1, K):
                s = kv_peer(i)
                kv_wait(ag, hbuf.at[s], s)
                acc = acc + dot(hbuf[s], wd_v[pl.ds(pl.multiple_of(s * CW, LANES), CW), :])
        else:
            acc = jnp.zeros((RP, wd_v.shape[1]), F32)
            for s in range(nown):
                pl.when(me != s)(functools.partial(kv_wait, ag, hbuf.at[s], s))
                acc = acc + dot(hbuf[s], wd_v[s * CW : (s + 1) * CW, :])
        return acc, more

    def tp_sum(phase, acc, send, buf):
        send[...] = acc.astype(BF16)
        for i in range(1, T):
            cp = tp_copy(phase, send, buf.at[mt], tp_peer(i))
            cp.start()
            sends.append((None, None, cp))
        buf[mt] = send[...]
        for i in range(1, T):
            tp_wait(phase, buf.at[tp_peer(i)], tp_peer(i))
        tot = buf[0].astype(F32)
        for t in range(1, T):
            tot = tot + buf[t].astype(F32)
        return tot

    def rest_of_loads():
        proj = [load(wq, wq_v), load(wk, wk_v), load(wv, wv_v)]
        keys = load_seqs(ck, ck_v)
        values = load_seqs(cv, cv_v)
        proj_out = [load(wo, wo_v)]
        in2 = load_cols(wg2, wg2_v) + load_cols(wu2, wu2_v)
        down2 = load_rows(wd2, wd2_v)
        return proj, keys, values, proj_out, in2, down2

    acc, (proj, keys, values, proj_out, in2, down2) = feed_forward(
        0, SQ1, x, g1, in1, wg1_v, wu1_v, down1, wd1_v, rs_send1, rs_recv1, hid1, RS1, AG1, rest_of_loads)
    x = (x.astype(F32) + 0.5 * tp_sum(SUM1, acc, sum1_send, sum1)).astype(BF16)

    scaled, squares = scaled_rows(x, gm)
    send_squares(1, SQM, squares, NC)
    wait_all(proj)
    pq = dot(scaled, wq_v[...])
    for n in range(NC):
        h, half = n // halves, n % halves
        q_send[n] = pq[half * 16 : half * 16 + 16, h * HEAD_DIM : (h + 1) * HEAD_DIM].astype(BF16)

    def to_owners(phase, send, recv):
        for i in range(1, K):
            j = kv_peer(i)
            cp = kv_copy(phase, send.at[j], recv.at[me], j)
            guarded(NC, j, cp.start)
            sends.append((NC, j, cp))

    def gather_chunks(phase, buf):
        for n in range(NC):
            pl.when(me != n)(functools.partial(kv_wait, phase, buf.at[n], n))

    to_owners(RSQ, q_send, q_recv)
    pk, pvv, plog = dot(scaled, wk_v[...]), dot(scaled, wv_v[...]), dot(scaled, fwx[...])
    for n in range(NC):
        h, half = n // halves, n % halves
        r, l = slice(half * 16, half * 16 + 16), slice(h * HEAD_DIM, (h + 1) * HEAD_DIM)
        k_send[n, 0] = pk[r, l].astype(BF16)
        k_send[n, 1] = pvv[r, l].astype(BF16)
        k_send[n, 2] = hi_lo(plog[r, h * HEAD_DIM : h * HEAD_DIM + 1], 16)
    to_owners(RSK, k_send, k_recv)
    factor = HEAD_DIM ** (-0.5)
    my_head = mt * heads + lax.rem(me, NC) // halves
    mine = lax.rem(me, NC)

    def own_query():
        rscale = row_scale(1, SQM)
        first_half = jnp.broadcast_to(lax.rem(mine, halves) == 0, (16, 1))
        rscale = jnp.where(first_half, rscale[0:16], rscale[RP - 16 : RP])
        tot = q_send[mine].astype(F32)
        for i in range(1, K):
            s = kv_peer(i)
            kv_wait(RSQ, q_recv.at[s], s)
            tot = tot + q_recv[s].astype(F32)
        q_buf[mine] = (tot * rscale).astype(BF16)
        for i in range(1, K):
            kv_copy(AGQ, q_buf.at[mine], q_buf.at[mine], kv_peer(i)).start()
        rows[0] = jnp.broadcast_to(rscale, (16, LANES))

    def own_fresh():
        tot = [k_send[mine, p].astype(F32) for p in range(3)]
        for i in range(1, K):
            s = kv_peer(i)
            kv_wait(RSK, k_recv.at[s], s)
            tot = [t + k_recv[s, p].astype(F32) for p, t in enumerate(tot)]
        rscale = rows[0]
        q32 = q_buf[mine].astype(F32)
        k32 = (tot[0] * rscale).astype(BF16).astype(F32)
        v32 = (tot[1] * rscale).astype(BF16).astype(F32)
        logit = from_hi_lo(tot[2]) * rscale + fb[my_head]
        own_score = jnp.broadcast_to(jnp.sum(q32 * k32, axis=1, keepdims=True) * factor, (16, LANES))
        return own_score, v32, jnp.minimum(logit, 0.0) - jnp.log(1.0 + jnp.exp(-jnp.abs(logit)))

    guarded(NC, me, own_query)
    for i in range(1, K):
        sends.append((NC, me, kv_copy(AGQ, q_buf.at[mine], q_buf.at[mine], kv_peer(i))))
    wait_all(keys)
    gather_chunks(AGQ, q_buf)
    for n in range(NC):
        h, half = n // halves, n % halves
        q_all[half * 16 : half * 16 + 16, h * HEAD_DIM : (h + 1) * HEAD_DIM] = q_buf[n].astype(F32)

    sel = lax.broadcasted_iota(jnp.int32, (SUB, width), 0) == lax.broadcasted_iota(jnp.int32, (SUB, width), 1) // HEAD_DIM
    for b in range(R):
        qb = jnp.where(sel, jnp.broadcast_to(q_all[b : b + 1, :], (SUB, width)), 0.0).astype(BF16)
        s = lax.dot_general(qb, ck_v[b], (((1,), (1,)), ((), ())), preferred_element_type=F32)
        s = s * factor + bias[b * SUB : (b + 1) * SUB, :]
        sc[b * SUB : (b + 1) * SUB, :] = jnp.where(place < lens[b], s, FLOOR)
    s = sc[...]
    top = jnp.max(s, axis=1, keepdims=True)
    weights = jnp.where(s > 0.5 * FLOOR, jnp.exp(s - top), 0.0)
    mass = jnp.sum(weights, axis=1, keepdims=True)
    sc[...] = weights
    lane = lax.broadcasted_iota(jnp.int32, stat.shape, 1)
    lane = lane % (LANES // 2)
    stat[...] = jnp.where(lane < 16, top, jnp.where(lane < 32, mass, total[...]))
    wait_all(values)
    for b in range(R):
        part = dot(sc[b * SUB : (b + 1) * SUB, :].astype(BF16), cv_v[b])
        for h in range(heads):
            pv[h, b * SUB : (b + 1) * SUB, :] = part[:, h * HEAD_DIM : (h + 1) * HEAD_DIM]
    for n in range(NC):
        h, half = n // halves, n % halves
        picked = pl.ds(half * 16 * SUB + h, 16, stride=SUB)
        a_send[n] = pv.at[h][picked, :].astype(BF16)
        st = stat[picked, :]
        left = lax.broadcasted_iota(jnp.int32, (SUB, LANES), 1) < LANES // 2
        s_send[n] = jnp.where(left, st[0:SUB], st[SUB : 2 * SUB])

    to_owners(RSS, s_send, s_recv)
    to_owners(RSA, a_send, a_recv)

    def own_attended():
        own_score, fresh_value, fresh_gate = own_fresh()
        a_recv[me] = a_send[mine]
        s_recv[me] = s_send[mine]
        for i in range(1, K):
            kv_wait(RSS, s_recv.at[kv_peer(i)], kv_peer(i))
            kv_wait(RSA, a_recv.at[kv_peer(i)], kv_peer(i))
        ahead = fresh_gate
        tops = [None] * K
        for s in reversed(range(K)):
            st = s_recv[s]
            tops[s] = unpack_column(st, 2) + ahead
            ahead = ahead + unpack_column(st, 2, 32)
        peak = own_score
        for s in range(K):
            peak = jnp.maximum(peak, tops[s])
        fresh = jnp.exp(own_score - peak)
        num, den = fresh * fresh_value, fresh
        for s in range(K):
            keep = jnp.exp(tops[s] - peak)
            num = num + keep * a_recv[s].astype(F32)
            den = den + keep * unpack_column(s_recv[s], 2, 16)
        att[mine] = (num / den).astype(BF16)
        for i in range(1, K):
            kv_copy(AGA, att.at[mine], att.at[mine], kv_peer(i)).start()

    guarded(NC, me, own_attended)
    for i in range(1, K):
        sends.append((NC, me, kv_copy(AGA, att.at[mine], att.at[mine], kv_peer(i))))
    wait_all(proj_out)
    gather_chunks(AGA, att)
    for n in range(NC):
        h, half = n // halves, n % halves
        att_all[half * 16 : half * 16 + 16, h * HEAD_DIM : (h + 1) * HEAD_DIM] = att[n]
    acc = dot(att_all[...], wo_v[...])
    x = (x.astype(F32) + tp_sum(SUM2, acc, sum2_send, sum2)).astype(BF16)

    acc, _ = feed_forward(
        2, SQ2, x, g2, in2, wg2_v, wu2_v, down2, wd2_v, rs_send2, rs_recv2, hid2, RS2, AG2, lambda: None)

    if c["gathered"]:
        tot = tp_sum(SUM3, acc, fin_send, fin_recv)
        out[...] = (x.astype(F32) + 0.5 * tot).astype(BF16)[0:R]
    else:
        cols = hid.shape[1]
        for t in range(T):
            fin_send[t] = acc[:, t * cols : (t + 1) * cols]
            fin_x[t] = x[:, t * cols : (t + 1) * cols]
        for i in range(1, T):
            cp = tp_copy(SUM3, fin_send.at[tp_peer(i)], fin_recv.at[mt], tp_peer(i))
            cp.start()
            sends.append((None, None, cp))
        fin_recv[mt] = fin_send[mt]
        for i in range(1, T):
            tp_wait(SUM3, fin_recv.at[tp_peer(i)], tp_peer(i))
        tot = fin_recv[0]
        for t in range(1, T):
            tot = tot + fin_recv[t]
        out[...] = (fin_x[mt].astype(F32) + 0.5 * tot).astype(BF16)[0:R]

    for limit, who, cp in sends:
        if limit is None:
            cp.wait_send()
        else:
            guarded(limit, who, cp.wait_send)


def local(
    K, T,
    hidden_rows, first_gain, first_gate, first_up, first_down, mix_gain,
    query_weight, key_weight, value_weight, forget_weight, forget_bias, out_weight,
    second_gain, second_gate, second_up, second_down,
    cache_keys, cache_values, cache_gates, lengths,
):
    R, cols = hidden_rows.shape
    Dl = first_gate.shape[0]
    gathered = cols % LANES != 0
    RP = up_to(R, 16)
    width = query_weight.shape[1]
    heads = width // HEAD_DIM
    span = cache_keys.shape[1]
    ff = up_to(first_gate.shape[1], LANES)
    short = ff - first_gate.shape[1]
    if short:
        first_gate, first_up, second_gate, second_up = (
            jnp.pad(w, ((0, 0), (0, short))) for w in (first_gate, first_up, second_gate, second_up))
        first_down, second_down = (jnp.pad(w, ((0, short), (0, 0))) for w in (first_down, second_down))
    tiles = ff // LANES
    CW = up_to(tiles, K) // K * LANES
    nown = -(-ff // CW)
    ffc = nown * CW
    NC = heads * (RP // 16)
    assert NC <= K and heads <= SUB
    rows_in = lax.all_gather(hidden_rows, "tp", axis=1, tiled=True) if gathered else hidden_rows
    c = dict(K=K, T=T, R=R, RP=RP, ff=ff, CW=CW, nown=nown, heads=heads, span=span, width=width,
             features=Dl * K, gathered=gathered, head_total=forget_bias.shape[0])
    xc = rows_in.shape[1]
    vm = pltpu.VMEM
    msg = 2 * CW
    scratch = [
        vm((Dl, ffc), BF16), vm((Dl, ffc), BF16), vm((ffc, Dl), BF16),
        vm((Dl, width), BF16), vm((Dl, width), BF16), vm((Dl, width), BF16), vm((width, Dl), BF16),
        vm((Dl, ffc), BF16), vm((Dl, ffc), BF16), vm((ffc, Dl), BF16),
        vm((R, span, width), BF16), vm((R, span, width), BF16),
        vm((T, RP, xc), BF16), vm((K, RP, msg), BF16), vm((K, RP, msg), BF16), vm((K, RP, CW), BF16),
        vm((RP, Dl), BF16), vm((T, RP, Dl), BF16),
        vm((3, SUB, LANES), F32), vm((3, K, SUB, LANES), F32),
        vm((K, 16, LANES), BF16), vm((K, 16, LANES), BF16),
        vm((K, 3, 16, LANES), BF16), vm((K, 3, 16, LANES), BF16), vm((NC, 16, LANES), BF16), vm((RP, width), F32),
        vm((Dl, width), BF16), vm((RP * SUB, span), F32), vm((RP * SUB, span), F32), vm((RP * SUB, LANES), F32),
        vm((RP * SUB, span), F32), vm((heads, RP * SUB, LANES), F32), vm((RP * SUB, LANES), F32),
        vm((K, 16, LANES), BF16), vm((K, 16, LANES), BF16),
        vm((K, SUB, LANES), F32), vm((K, SUB, LANES), F32), vm((NC, 16, LANES), BF16), vm((RP, width), BF16),
        vm((RP, Dl), BF16), vm((T, RP, Dl), BF16),
        vm((K, RP, msg), BF16), vm((K, RP, msg), BF16), vm((K, RP, CW), BF16),
        vm((RP, Dl), BF16) if gathered else vm((T, RP, xc), F32),
        vm((T, RP, Dl), BF16) if gathered else vm((T, RP, xc), F32),
        vm((T, RP, xc), BF16), vm((1, 16, LANES), F32),
        pltpu.SemaphoreType.DMA((48,)),
        pltpu.SemaphoreType.DMA((13, K)), pltpu.SemaphoreType.DMA((13, K)),
        pltpu.SemaphoreType.DMA((4, T)), pltpu.SemaphoreType.DMA((4, T)),
    ]
    in_vmem = pl.BlockSpec(memory_space=pltpu.VMEM)
    in_smem = pl.BlockSpec(memory_space=pltpu.SMEM)
    anywhere = pl.BlockSpec(memory_space=pl.ANY)
    result = pl.pallas_call(
        functools.partial(kernel, c),
        out_shape=jax.ShapeDtypeStruct((R, xc), BF16),
        in_specs=[in_vmem] * 6 + [in_smem] * 2 + [anywhere] * 12,
        out_specs=in_vmem,
        scratch_shapes=scratch,
        compiler_params=pltpu.CompilerParams(
            collective_id=0, has_side_effects=True, vmem_limit_bytes=60 * 1024 * 1024),
        name="layer",
    )(
        rows_in, first_gain.reshape(1, Dl), mix_gain.reshape(1, Dl), second_gain.reshape(1, Dl),
        forget_weight, cache_gates, forget_bias, lengths,
        first_gate, first_up, first_down, query_weight, key_weight, value_weight, out_weight,
        second_gate, second_up, second_down, cache_keys, cache_values,
    )
    if gathered:
        return lax.dynamic_slice_in_dim(result, lax.axis_index("tp") * cols, cols, 1)
    return result


def solution(mesh):
    return jax.shard_map(
        functools.partial(local, mesh.shape["kv"], mesh.shape["tp"]),
        mesh=mesh,
        in_specs=(
            P(None, ("kv", "tp")),
            P("kv"),
            P("kv", "tp"),
            P("kv", "tp"),
            P("tp", "kv"),
            P("kv"),
            P("kv", "tp"),
            P("kv", "tp"),
            P("kv", "tp"),
            P("kv", None),
            P(),
            P("tp", "kv"),
            P("kv"),
            P("kv", "tp"),
            P("kv", "tp"),
            P("tp", "kv"),
            P(None, "kv", "tp"),
            P(None, "kv", "tp"),
            P(None, "tp", "kv"),
            P(),
        ),
        out_specs=P(None, ("kv", "tp")),
        check_vma=False,
    )
```
